512 devices in a mesh: grp: 2 (over y), kv: 64 (over z, core), tp: 4 (over x).
Axes of the slice: x: 4, y: 2, z: 32, core: 2. Of those that a mesh axis runs over, the one named last changes fastest.
The devices are a block of a 4x8x32 slice.
Arguments:
- tokens: bfloat16 [65536, 2048], P(('grp', 'kv')), parts along dimension 0, may hold values from -72 to 72
- w_query: bfloat16 [2048, 1024], P(None, 'tp'), may hold values from -0.125 to 0.125
- w_key: bfloat16 [2048, 256], P(None, 'tp'), may hold values from -0.125 to 0.125
- w_value: bfloat16 [2048, 256], P(None, 'tp'), may hold values from -0.125 to 0.125
- w_out: bfloat16 [1024, 2048], P('tp'), may hold values from -0.1875 to 0.1875
- selection: int32 [4, 1024, 32], P('tp', ('grp', 'kv')), parts along dimension 1, may hold values from -1 to 511, as said below
Outputs:
- attended_out: bfloat16 [65536, 2048], P(('grp', 'kv', 'tp')), parts along dimension 0
The draws below stay inside these ranges and needn't reach their ends.
There are 2 independent parts, one for each index of `grp`. The reference program is written for one: setup_inputs(seed, part) draws one part's arguments, and reference() takes and returns one part's arrays. A program takes and returns all parts, laid end to end along the dimension named above; an argument that names none is the same for every part. Nothing has to cross between parts.
Inputs may be any that keep to these rules, and one draw needn't show every extreme that they name: `selection`: entry 0 is the query block's own index; the others are distinct indices of earlier blocks, then -1 for unused entries. For one key head, the query blocks of one device's range together choose at most 2 distinct blocks of any other device's range, and some device reaches 2 in every draw.
All inputs are finite; a program needn't handle non-finite values.
Results may differ from the reference program's by a relative error of at most 0.028.
The reference program's roundings to bfloat16 on the way (of `queries`, `keys`, `values`, `weights` and `attended`) count: a program that leaves them out, or rounds other values in their place, can miss the bound.
Values may be sent and summed in bfloat16 or wider, within the bound.
No kernel may reach another device: no remote copies, remote signals or barrier semaphores. Data moves between devices by JAX's collectives and lax.ppermute only.
A program may use at most 128 MiB of HBM per device.

```python
import jax
import jax.numpy as jnp
from jax import lax

D = 2048
HEADS = 16
KV_HEADS = 4
HEAD_DIM = 64
BLOCK = 64
TOPK = 32
CAP = 2
QB_DEV = 8
TOKENS = 32768
NQB = 512
N_TP = 4


def draw_tokens(key, part):
    normal_draw = jax.random.normal(jax.random.fold_in(key, 11), (TOKENS, D), jnp.float32)
    normal_draw = jnp.clip(normal_draw, -6.0, 6.0)
    return normal_draw.astype(jnp.bfloat16)


def draw_selection(key, part):
    per_dev = QB_DEV
    total_blocks = NQB
    devices = total_blocks // per_dev
    pair_score = jax.random.randint(jax.random.fold_in(key, 21), (KV_HEADS, devices, devices, per_dev), 0, 1 << 20) * per_dev + jnp.arange(per_dev)
    rank_in = jnp.sum((pair_score[..., None, :] > pair_score[..., :, None]).astype(jnp.int32), axis=-1)
    in_pair = rank_in < CAP
    popular = jax.random.randint(jax.random.fold_in(key, 22), (KV_HEADS, total_blocks), 0, 4) * 300
    noise_int = jax.random.randint(jax.random.fold_in(key, 23), (KV_HEADS, total_blocks, total_blocks), 0, 1000)
    block_ids = jnp.arange(total_blocks)
    owner_ids = block_ids // per_dev
    within_ids = block_ids % per_dev
    dev_of = block_ids // per_dev
    slot_of = block_ids % per_dev
    pair_here = in_pair[:, dev_of[:, None], owner_ids[None, :], within_ids[None, :]]
    remote = (owner_ids[None, :] < dev_of[:, None])[None] & pair_here
    earlier = (owner_ids[None, :] == dev_of[:, None]) & (within_ids[None, :] < slot_of[:, None])
    candidate = remote | earlier[None]
    forced = (owner_ids[None, :] == dev_of[:, None] - 1) & (slot_of == 1)[:, None] | (owner_ids[None, :] == dev_of[:, None] - devices // 2) & (slot_of == 2)[:, None]
    value_int = noise_int + popular[:, None, :] + 4096 * forced[None].astype(jnp.int32)
    score_int = jnp.where(candidate, value_int * total_blocks + block_ids, -1 - block_ids)
    top_scores, top_index = lax.top_k(score_int, TOPK - 1)
    others = jnp.where(top_scores >= 0, top_index, -1)
    own_block = jnp.broadcast_to(block_ids[None, :, None], (KV_HEADS, total_blocks, 1))
    return jnp.concatenate([own_block, others], axis=-1).astype(jnp.int32)


def level_of(key, extent, split, low, high):
    def one(axis_at, blocks):
        heights = jax.random.uniform(jax.random.fold_in(jax.random.fold_in(key, 6), axis_at), (blocks,), jnp.float32, low / len(split), high / len(split))
        return jnp.repeat(jnp.exp(heights), extent[axis_at] // blocks).reshape((-1,) + (1,) * (len(extent) - axis_at - 1))

    factor_of = one(*split[0])
    for cut in split[1:]:
        factor_of = factor_of * one(*cut)
    return factor_of


def noise(own_key, extent, deviation, bound, shards=(), kind=jnp.bfloat16):
    level = level_of(own_key, extent, shards, -0.22, 0.18) if shards else 1.0
    array = jax.random.normal(own_key, extent, jnp.float32) * deviation * level
    return jnp.minimum(jnp.maximum(array, -bound), bound).astype(kind)


def setup_inputs(seed: int = 0, part: int = 0) -> dict:
    splits = jax.random.split(jax.random.key(seed), 7)
    part_splits = jax.random.split(jax.random.fold_in(splits[6], part), 7)
    tokens = draw_tokens(jax.random.fold_in(jax.random.fold_in(splits[6], part), 71), part)
    w_query = noise(splits[1], (D, HEADS * HEAD_DIM), D ** -0.5, 0.125, ((1, 4),))
    w_key = noise(splits[2], (D, KV_HEADS * HEAD_DIM), D ** -0.5, 0.125, ((1, 4),))
    w_value = noise(splits[3], (D, KV_HEADS * HEAD_DIM), D ** -0.5, 0.125, ((1, 4),))
    w_out = noise(splits[4], (HEADS * HEAD_DIM, D), (HEADS * HEAD_DIM) ** -0.5, 0.1875, ((0, 4),))
    selection = draw_selection(jax.random.fold_in(jax.random.fold_in(splits[6], part), 71), part)
    return {"tokens": tokens, "w_query": w_query, "w_key": w_key, "w_value": w_value, "w_out": w_out, "selection": selection}


ROPE_BASE = 500000.0


def rotate(head_rows, positions):
    half = head_rows.shape[-1] // 2
    freqs = ROPE_BASE ** (-jnp.arange(half, dtype=jnp.float32) / half)
    angles = positions[:, None, None] * freqs
    cosine = jnp.cos(angles)
    sine = jnp.sin(angles)
    first = head_rows[..., :half]
    second = head_rows[..., half:]
    return jnp.concatenate([first * cosine - second * sine, second * cosine + first * sine], axis=-1)


def reference(tokens, w_query, w_key, w_value, w_out, selection):
    length = tokens.shape[0]
    positions = jnp.arange(length).astype(jnp.float32)
    queries = rotate(jnp.dot(tokens, w_query, preferred_element_type=jnp.float32).reshape(length, HEADS, HEAD_DIM), positions).astype(jnp.bfloat16)
    keys = rotate(jnp.dot(tokens, w_key, preferred_element_type=jnp.float32).reshape(length, KV_HEADS, HEAD_DIM), positions).astype(jnp.bfloat16)
    values = jnp.dot(tokens, w_value, preferred_element_type=jnp.float32).astype(jnp.bfloat16)
    key_blocks = jnp.transpose(keys.reshape(NQB, BLOCK, KV_HEADS, HEAD_DIM), (2, 0, 1, 3))
    value_blocks = jnp.transpose(values.reshape(NQB, BLOCK, KV_HEADS, HEAD_DIM), (2, 0, 1, 3))
    group = HEADS // KV_HEADS
    head_ids = jnp.arange(KV_HEADS)[:, None]
    offsets = jnp.arange(BLOCK).astype(jnp.int32)
    score_scale = HEAD_DIM ** -0.5

    def one_block(block_id):
        query_rows = lax.dynamic_slice_in_dim(queries, block_id * BLOCK, BLOCK, 0).reshape(BLOCK, KV_HEADS, group, HEAD_DIM)
        chosen_ids = lax.dynamic_index_in_dim(selection, block_id, 1, keepdims=False)
        safe_ids = jnp.maximum(chosen_ids, 0)
        picked_keys = key_blocks[head_ids, safe_ids].reshape(KV_HEADS, TOPK * BLOCK, HEAD_DIM)
        picked_values = value_blocks[head_ids, safe_ids].reshape(KV_HEADS, TOPK * BLOCK, HEAD_DIM)
        scores = jnp.einsum('qhgd,hkd->hgqk', query_rows.astype(jnp.float32), picked_keys.astype(jnp.float32)) * score_scale
        key_pos = (chosen_ids[:, :, None] * BLOCK + offsets).reshape(KV_HEADS, TOPK * BLOCK)
        live_keys = jnp.repeat(chosen_ids >= 0, BLOCK, axis=1)
        query_pos = block_id * BLOCK + offsets
        allowed = live_keys[:, None, None, :] & (key_pos[:, None, None, :] <= query_pos[None, None, :, None])
        scores = jnp.where(allowed, scores, -jnp.inf)
        top_score = jnp.max(scores, axis=-1, keepdims=True)
        expo = jnp.exp(scores - top_score)
        weights = (expo / jnp.sum(expo, axis=-1, keepdims=True)).astype(jnp.bfloat16)
        attended = jnp.einsum('hgqk,hkd->qhgd', weights.astype(jnp.float32), picked_values.astype(jnp.float32)).astype(jnp.bfloat16)
        return attended.reshape(BLOCK, HEADS * HEAD_DIM)

    attended = lax.map(one_block, jnp.arange(NQB).astype(jnp.int32)).reshape(length, HEADS * HEAD_DIM)
    width = HEADS * HEAD_DIM // N_TP
    summed = jnp.zeros((length, D), jnp.float32)
    for group_id in range(N_TP):
        partial_out = jnp.dot(attended[:, group_id * width:(group_id + 1) * width], w_out[group_id * width:(group_id + 1) * width], preferred_element_type=jnp.float32).astype(jnp.bfloat16)
        summed = summed + lax.optimization_barrier(partial_out).astype(jnp.float32)
    return summed.astype(jnp.bfloat16)
```

```python
import functools

import jax
import jax.numpy as jnp
from jax import lax
from jax.experimental import pallas as pl
from jax.experimental.pallas import tpu as pltpu
from jax.sharding import PartitionSpec as P

HEAD_DIM = 64
BLOCK = 64
ROPE_BASE = 500000.0
LANES = 2 * HEAD_DIM
HALF = HEAD_DIM // 2


def encode(x):
    mag = jnp.abs(x)
    live = mag >= 2.0**-126
    safe = jnp.where(live, mag, 1.0)
    exponent = jnp.floor(jnp.log2(safe))
    exponent = jnp.clip(exponent, -126.0, 127.0)
    half_exp = jnp.floor(exponent * 0.5)
    ratio = safe * jnp.exp2(-half_exp) * jnp.exp2(half_exp - exponent)
    code = (exponent + 126.0) * 128.0 + jnp.floor(ratio * 128.0 + 0.5)
    code = jnp.where(live, code, 0.0)
    return jnp.where(x < 0, -code, code).astype(jnp.int32).astype(jnp.int16)


def decode(code):
    signed = code.astype(jnp.int32).astype(jnp.float32)
    level = jnp.abs(signed) * (1.0 / 128.0)
    whole = jnp.floor(level)
    mag = (level - whole + 1.0) * jnp.exp2(whole - 127.0)
    return jnp.where(signed < 0, -mag, mag).astype(jnp.bfloat16)


def swap_halves(x, lane):
    return jnp.where(
        lane % HEAD_DIM < HALF,
        pltpu.roll(x, LANES - HALF, 1),
        pltpu.roll(x, HALF, 1),
    )


def project_body(tok_ref, wq_ref, wk_ref, wv_ref, cos_ref, sin_ref, code_ref, q_ref, wkv_ref):
    @pl.when(pl.program_id(0) == 0)
    def _():
        wkv_ref[:, :HEAD_DIM] = wk_ref[...]
        wkv_ref[:, HEAD_DIM:] = wv_ref[...]

    tok = tok_ref[...]
    rows = tok.shape[0]
    lane = lax.broadcasted_iota(jnp.int32, (rows, LANES), 1)
    cosine = cos_ref[...]
    sine = sin_ref[...]
    kv = jnp.dot(tok, wkv_ref[...], preferred_element_type=jnp.float32)
    is_key = lane < HEAD_DIM
    kv = jnp.where(is_key, kv * cosine + swap_halves(kv, lane) * sine, kv)
    code_ref[...] = encode(kv.astype(jnp.bfloat16).astype(jnp.float32))
    q_all = jnp.dot(tok, wq_ref[...], preferred_element_type=jnp.float32)
    heads = q_all.shape[1] // HEAD_DIM
    for pair in range(heads // 2):
        q = q_all[:, pair * LANES : (pair + 1) * LANES]
        q = q * cosine + swap_halves(q, lane) * sine
        q = q.astype(jnp.bfloat16).astype(jnp.float32) * HEAD_DIM**-0.5
        for odd in range(2):
            one = pltpu.roll(q, HEAD_DIM, 1) if odd else q
            one = jnp.where(is_key, one, 0.0).astype(jnp.bfloat16)
            for b in range(rows // BLOCK):
                at = (2 * pair + odd) * BLOCK
                q_ref[b, at : at + BLOCK, :] = one[b * BLOCK : (b + 1) * BLOCK]


def project(tokens, w_query, w_key, w_value, cosine, sine):
    rows, width = tokens.shape
    qcols = w_query.shape[1]
    heads = qcols // HEAD_DIM
    tile = 128
    return pl.pallas_call(
        project_body,
        grid=(rows // tile,),
        in_specs=[
            pl.BlockSpec((tile, width), lambda i: (i, 0)),
            pl.BlockSpec((width, qcols), lambda i: (0, 0)),
            pl.BlockSpec((width, HEAD_DIM), lambda i: (0, 0)),
            pl.BlockSpec((width, HEAD_DIM), lambda i: (0, 0)),
            pl.BlockSpec((tile, LANES), lambda i: (i, 0)),
            pl.BlockSpec((tile, LANES), lambda i: (i, 0)),
        ],
        out_specs=[
            pl.BlockSpec((tile, LANES), lambda i: (i, 0)),
            pl.BlockSpec((tile // BLOCK, heads * BLOCK, LANES), lambda i: (i, 0, 0)),
        ],
        out_shape=[
            jax.ShapeDtypeStruct((rows, LANES), jnp.int16),
            jax.ShapeDtypeStruct((rows // BLOCK, heads * BLOCK, LANES), jnp.bfloat16),
        ],
        scratch_shapes=[pltpu.VMEM((width, LANES), jnp.bfloat16)],
        compiler_params=pltpu.CompilerParams(dimension_semantics=("arbitrary",)),
        name="project",
    )(tokens, w_query, w_key, w_value, cosine, sine)


def attend_body(sel_ref, q_ref, bias_ref, table_ref, out_ref, kv_ref, s_ref, p_ref, *, topk):
    b = pl.program_id(0)
    for t in range(topk):
        at = pl.multiple_of(jnp.maximum(sel_ref[b, t], 0) * BLOCK, BLOCK)
        kv_ref[t * BLOCK : (t + 1) * BLOCK, :] = decode(table_ref[pl.ds(at, BLOCK), :])
    q = q_ref[0]
    rows = q.shape[0]
    s_ref[...] = lax.dot_general(
        q, kv_ref[...], (((1,), (1,)), ((), ())), preferred_element_type=jnp.float32
    )
    chunk = 32
    bias = bias_ref[0]
    sums = []
    for r in range(0, rows, chunk):
        s = s_ref[r : r + chunk, :] + bias
        row = lax.broadcasted_iota(jnp.int32, (chunk, LANES), 0) + r % BLOCK
        col = lax.broadcasted_iota(jnp.int32, (chunk, LANES), 1)
        first = jnp.where((col < BLOCK) & (col > row), -jnp.inf, s[:, :LANES])
        s = jnp.concatenate([first, s[:, LANES:]], axis=1)
        e = jnp.exp(s - jnp.max(s, axis=1, keepdims=True))
        sums.append(jnp.sum(e, axis=1, keepdims=True))
        p_ref[r : r + chunk, :] = e.astype(jnp.bfloat16)
    o = jnp.dot(p_ref[...], kv_ref[...], preferred_element_type=jnp.float32)
    o = o / jnp.concatenate(sums, axis=0)
    lane = lax.broadcasted_iota(jnp.int32, (BLOCK, LANES), 1)
    for pair in range(rows // BLOCK // 2):
        even = o[2 * pair * BLOCK : (2 * pair + 1) * BLOCK]
        odd = o[(2 * pair + 1) * BLOCK : (2 * pair + 2) * BLOCK]
        both = jnp.where(lane < HEAD_DIM, pltpu.roll(even, HEAD_DIM, 1), odd)
        out_ref[:, pair * LANES : (pair + 1) * LANES] = both.astype(jnp.bfloat16)


def attend(chosen, queries, bias, table):
    blocks, topk = chosen.shape
    rows = queries.shape[1]
    cols = rows // BLOCK * HEAD_DIM
    keys = topk * BLOCK
    return pl.pallas_call(
        functools.partial(attend_body, topk=topk),
        grid_spec=pltpu.PrefetchScalarGridSpec(
            num_scalar_prefetch=1,
            grid=(blocks,),
            in_specs=[
                pl.BlockSpec((1, rows, LANES), lambda i, s: (i, 0, 0)),
                pl.BlockSpec((1, 1, keys), lambda i, s: (i, 0, 0)),
                pl.BlockSpec(memory_space=pltpu.VMEM),
            ],
            out_specs=pl.BlockSpec((BLOCK, cols), lambda i, s: (i, 0)),
            scratch_shapes=[
                pltpu.VMEM((keys, LANES), jnp.bfloat16),
                pltpu.VMEM((rows, keys), jnp.float32),
                pltpu.VMEM((rows, keys), jnp.bfloat16),
            ],
        ),
        out_shape=jax.ShapeDtypeStruct((blocks * BLOCK, cols), jnp.bfloat16),
        compiler_params=pltpu.CompilerParams(
            dimension_semantics=("arbitrary",), vmem_limit_bytes=40 * 1024 * 1024
        ),
        name="attend",
    )(chosen, queries, bias, table)


def combine_body(x_ref, w_ref, out_ref):
    total = None
    for g in range(x_ref.shape[0]):
        part = jnp.dot(x_ref[g], w_ref[g], preferred_element_type=jnp.float32)
        part = part.astype(jnp.bfloat16).astype(jnp.float32)
        total = part if total is None else total + part
    out_ref[...] = total.astype(jnp.bfloat16)


def combine(parts, weights):
    peers, rows, depth = parts.shape
    cols = weights.shape[2]
    tile = 512
    return pl.pallas_call(
        combine_body,
        grid=(cols // tile,),
        in_specs=[
            pl.BlockSpec((peers, rows, depth), lambda j: (0, 0, 0)),
            pl.BlockSpec((peers, depth, tile), lambda j: (0, 0, j)),
        ],
        out_specs=pl.BlockSpec((rows, tile), lambda j: (0, j)),
        out_shape=jax.ShapeDtypeStruct((rows, cols), jnp.bfloat16),
        name="combine",
    )(parts, weights)


def rope_tables(row_count):
    positions = (lax.axis_index("kv") * row_count + jnp.arange(row_count)).astype(jnp.float32)
    lane = jnp.arange(LANES)
    freqs = ROPE_BASE ** (-(lane % HALF).astype(jnp.float32) / HALF)
    angles = positions[:, None] * freqs
    sign = jnp.where(lane % HEAD_DIM < HALF, -1.0, 1.0)
    return jnp.cos(angles), jnp.sin(angles) * sign


def shards(tokens, w_query, w_key, w_value, w_out, selection):
    row_count = tokens.shape[0]
    peers = lax.axis_size("tp")
    cosine, sine = rope_tables(row_count)
    codes, queries = project(tokens, w_query, w_key, w_value, cosine, sine)
    table = lax.all_gather(codes, "kv", axis=0, tiled=True)
    w_all = lax.all_gather(w_out, "tp", axis=0, tiled=False)
    chosen = selection[0]
    bias = jnp.where(jnp.repeat(chosen >= 0, BLOCK, axis=1), 0.0, -jnp.inf)
    attended = attend(chosen, queries, bias[:, None, :], table)
    tiles = attended.reshape(peers, row_count // peers, attended.shape[1])
    arrived = lax.all_to_all(tiles, "tp", split_axis=0, concat_axis=0, tiled=True)
    return combine(arrived, w_all)


def solution(mesh):
    placed = (
        P(("grp", "kv"), None),
        P(None, "tp"),
        P(None, "tp"),
        P(None, "tp"),
        P("tp", None),
        P("tp", ("grp", "kv"), None),
    )
    return jax.shard_map(
        shards, mesh=mesh, in_specs=placed, out_specs=P(("grp", "kv", "tp"), None), check_vma=False
    )
```

```python
import jax
import jax.numpy as jnp
from jax import lax
from jax.experimental import pallas as pl
from jax.experimental.pallas import tpu as pltpu
from jax.sharding import PartitionSpec as P


HEAD_DIM = 64
BLOCK = 64
ROPE_BASE = 500000.0
LANES = 2 * HEAD_DIM
HALF = HEAD_DIM // 2


def encode(x):
    mag = jnp.abs(x)
    live = mag >= 2.0**-126
    safe = jnp.where(live, mag, 1.0)
    exponent = jnp.clip(jnp.floor(jnp.log2(safe)), -126.0, 126.0)
    half_exp = jnp.floor(exponent * 0.5)
    mantissa = safe * jnp.exp2(-half_exp) * jnp.exp2(half_exp - exponent)
    place = jnp.floor(mantissa * 128.0 - 127.5)
    carry = place >= 128.0
    place = jnp.where(carry, 0.0, place)
    exponent = jnp.where(carry, exponent + 1.0, exponent)
    code = (exponent + 1.0) * 256.0 + jnp.where(x < 0, 127.0 - place, 128.0 + place)
    return jnp.where(live, code, 128.0 - 126.0 * 256.0).astype(jnp.int32).astype(jnp.int16)


def decode(code):
    level = code.astype(jnp.int32).astype(jnp.float32) * (1.0 / 256.0)
    whole = jnp.floor(level)
    part = level - whole
    part = part - jnp.where(part < 0.5, 255.0 / 256.0, 0.0)
    return (part * jnp.exp2(whole)).astype(jnp.bfloat16)


def swap_halves(x, lane):
    return jnp.where(
        lane % HEAD_DIM < HALF,
        pltpu.roll(x, LANES - HALF, 1),
        pltpu.roll(x, HALF, 1),
    )


def turns(cos_ref, sin_ref, b):
    starts = cos_ref.shape[0] - BLOCK
    cos_at = cos_ref[b : b + 1, :]
    sin_at = sin_ref[b : b + 1, :]
    cos_in = cos_ref[starts:, :]
    sin_in = sin_ref[starts:, :]
    lane = lax.broadcasted_iota(jnp.int32, (BLOCK, LANES), 1)
    sign = jnp.where(lane % HEAD_DIM < HALF, -1.0, 1.0)
    return cos_at * cos_in - sin_at * sin_in, (sin_at * cos_in + cos_at * sin_in) * sign, lane


TILE = 4 * BLOCK
PART = 2 * BLOCK


def codes_body(
    tok_hbm, wk_hbm, wv_hbm, cos_hbm, sin_hbm, wo_hbm, code_hbm, sent_hbm,
    tok_ref, wkv_ref, cos_ref, sin_ref, code_ref, wo_ref, sems
):
    firsts = range(0, tok_ref.shape[0], PART)
    peers = sent_hbm.shape[0]
    at = iter(range(5 + 2 * len(firsts) + peers))
    small = [
        pltpu.make_async_copy(wk_hbm, wkv_ref.at[:HEAD_DIM], sems.at[next(at)]),
        pltpu.make_async_copy(wv_hbm, wkv_ref.at[HEAD_DIM:], sems.at[next(at)]),
        pltpu.make_async_copy(cos_hbm, cos_ref, sems.at[next(at)]),
        pltpu.make_async_copy(sin_hbm, sin_ref, sems.at[next(at)]),
    ]
    spans = [pl.ds(first, PART) for first in firsts]
    reads = [
        pltpu.make_async_copy(tok_hbm.at[span], tok_ref.at[span], sems.at[next(at)]) for span in spans
    ]
    writes = [
        pltpu.make_async_copy(code_ref.at[span], code_hbm.at[span], sems.at[next(at)]) for span in spans
    ]
    copies = [
        pltpu.make_async_copy(wo_ref, sent_hbm.at[peer], sems.at[next(at)]) for peer in range(peers)
    ]
    stage = pltpu.make_async_copy(wo_hbm, wo_ref, sems.at[next(at)])
    for move in small + reads[:1] + [stage] + reads[1:]:
        move.start()
    for move in small:
        move.wait()
    for first, read, write in zip(firsts, reads, writes):
        read.wait()
        if first == PART:
            stage.wait()
            for move in copies:
                move.start()
        kv_all = lax.dot_general(
            tok_ref[first : first + PART, :],
            wkv_ref[...],
            (((1,), (1,)), ((), ())),
            preferred_element_type=jnp.float32,
        )
        for at in range(0, PART, BLOCK):
            cosine, sine, lane = turns(cos_ref, sin_ref, (first + at) // BLOCK)
            kv = kv_all[at : at + BLOCK]
            kv = jnp.where(lane < HEAD_DIM, kv * cosine + swap_halves(kv, lane) * sine, kv)
            code_ref[first + at : first + at + BLOCK, :] = encode(
                kv.astype(jnp.bfloat16).astype(jnp.float32)
            )
        write.start()
    for move in writes + copies:
        move.wait()


def project_codes(tokens, w_key, w_value, cosine, sine, w_out, peers):
    rows, width = tokens.shape
    far = pl.BlockSpec(memory_space=pltpu.HBM)
    return pl.pallas_call(
        codes_body,
        in_specs=[far] * 6,
        out_specs=[far] * 2,
        out_shape=[
            jax.ShapeDtypeStruct((rows, LANES), jnp.int16),
            jax.ShapeDtypeStruct((peers, *w_out.shape), jnp.bfloat16),
        ],
        scratch_shapes=[
            pltpu.VMEM((rows, width), jnp.bfloat16),
            pltpu.VMEM((LANES, width), jnp.bfloat16),
            pltpu.VMEM(cosine.shape, jnp.float32),
            pltpu.VMEM(sine.shape, jnp.float32),
            pltpu.VMEM((rows, LANES), jnp.int16),
            pltpu.VMEM(w_out.shape, jnp.bfloat16),
            pltpu.SemaphoreType.DMA((5 + 2 * (rows // PART) + peers,)),
        ],
        compiler_params=pltpu.CompilerParams(vmem_limit_bytes=63 * 1024 * 1024),
        name="project_codes",
    )(tokens, w_key.T, w_value.T, cosine, sine, w_out)


def queries_body(tok_ref, wq_ref, cos_ref, sin_ref, q_ref):
    for first in range(0, tok_ref.shape[0], TILE):
        q_all = jnp.dot(
            tok_ref[first : first + TILE, :], wq_ref[...], preferred_element_type=jnp.float32
        )
        for at in range(0, TILE, BLOCK):
            b = (first + at) // BLOCK
            cosine, sine, lane = turns(cos_ref, sin_ref, b)
            for pair in range(q_all.shape[1] // LANES):
                q = q_all[at : at + BLOCK, pair * LANES : (pair + 1) * LANES]
                q = q * cosine + swap_halves(q, lane) * sine
                q = q.astype(jnp.bfloat16).astype(jnp.float32) * HEAD_DIM**-0.5
                even = 2 * pair * BLOCK
                odd = even + BLOCK
                q_ref[b, even:odd, :] = jnp.where(lane < HEAD_DIM, q, 0.0).astype(jnp.bfloat16)
                q_ref[b, odd : odd + BLOCK, :] = jnp.where(
                    lane < HEAD_DIM, pltpu.roll(q, HEAD_DIM, 1), 0.0
                ).astype(jnp.bfloat16)


def project_queries(tokens, w_query, cosine, sine):
    rows = tokens.shape[0]
    heads = w_query.shape[1] // HEAD_DIM
    whole = pl.BlockSpec(memory_space=pltpu.VMEM)
    return pl.pallas_call(
        queries_body,
        in_specs=[whole] * 4,
        out_specs=whole,
        out_shape=jax.ShapeDtypeStruct((rows // BLOCK, heads * BLOCK, LANES), jnp.bfloat16),
        compiler_params=pltpu.CompilerParams(vmem_limit_bytes=32 * 1024 * 1024),
        name="project_queries",
    )(tokens, w_query, cosine, sine)


SLOTS = 4


def attend_body(sel_ref, q_ref, table_ref, out_ref, *scratch):
    kv_refs, s_refs, p_refs = scratch[:SLOTS], scratch[SLOTS : 2 * SLOTS], scratch[2 * SLOTS :]
    blocks, topk = sel_ref.shape
    rows = q_ref.shape[1]
    keys = topk * BLOCK
    chunk = 16
    row = lax.broadcasted_iota(jnp.int32, (chunk, LANES), 0)
    col = lax.broadcasted_iota(jnp.int32, (chunk, LANES), 1)
    key_at = lax.broadcasted_iota(jnp.int32, (1, keys), 1)
    half_lane = lax.broadcasted_iota(jnp.int32, (BLOCK, LANES), 1) < HEAD_DIM

    def load(k, b):
        used = jnp.int32(0)
        for t in range(topk):
            block = sel_ref[b, t]
            used += (block >= 0).astype(jnp.int32)
            at = pl.multiple_of(jnp.maximum(block, 0) * BLOCK, BLOCK)
            kv_refs[k][t * BLOCK : (t + 1) * BLOCK, :] = decode(table_ref[pl.ds(at, BLOCK), :])
        return jnp.where(key_at < used * BLOCK, 0.0, -jnp.inf)

    def score(k, b):
        s_refs[k][...] = lax.dot_general(
            q_ref[b], kv_refs[k][...], (((1,), (1,)), ((), ())), preferred_element_type=jnp.float32
        )

    def soften(k, bias):
        sums = []
        for r in range(0, rows, chunk):
            s = s_refs[k][r : r + chunk, :] + bias
            first = jnp.where((col < BLOCK) & (col > row + r % BLOCK), -jnp.inf, s[:, :LANES])
            s = jnp.concatenate([first, s[:, LANES:]], axis=1)
            e = jnp.exp(s - jnp.max(s, axis=1, keepdims=True))
            sums.append(jnp.sum(e, axis=1, keepdims=True))
            p_refs[k][r : r + chunk, :] = e.astype(jnp.bfloat16)
        return jnp.concatenate(sums, axis=0)

    def finish(k, b, sums):
        o = jnp.dot(p_refs[k][...], kv_refs[k][...], preferred_element_type=jnp.float32) / sums
        at = pl.multiple_of(b * BLOCK, BLOCK)
        for pair in range(rows // BLOCK // 2):
            even = o[2 * pair * BLOCK : (2 * pair + 1) * BLOCK]
            odd = o[(2 * pair + 1) * BLOCK : (2 * pair + 2) * BLOCK]
            both = jnp.where(half_lane, pltpu.roll(even, HEAD_DIM, 1), odd)
            out_ref[pl.ds(at, BLOCK), pair * LANES : (pair + 1) * LANES] = both.astype(jnp.bfloat16)

    def step(i, _):
        first = i * SLOTS
        biases = [load(0, first)]
        score(0, first)
        for k in range(SLOTS):
            if k + 1 < SLOTS:
                biases.append(load(k + 1, first + k + 1))
            sums = soften(k, biases[k])
            if k + 1 < SLOTS:
                score(k + 1, first + k + 1)
            finish(k, first + k, sums)
        return 0

    lax.fori_loop(0, blocks // SLOTS, step, 0)


def attend(chosen, queries, table):
    blocks, topk = chosen.shape
    rows = queries.shape[1]
    cols = rows // BLOCK * HEAD_DIM
    keys = topk * BLOCK
    whole = pl.BlockSpec(memory_space=pltpu.VMEM)
    return pl.pallas_call(
        attend_body,
        in_specs=[pl.BlockSpec(memory_space=pltpu.SMEM), whole, whole],
        out_specs=whole,
        out_shape=jax.ShapeDtypeStruct((blocks * BLOCK, cols), jnp.bfloat16),
        scratch_shapes=[pltpu.VMEM((keys, LANES), jnp.bfloat16) for _ in range(SLOTS)]
        + [pltpu.VMEM((rows, keys), jnp.float32) for _ in range(SLOTS)]
        + [pltpu.VMEM((rows, keys), jnp.bfloat16) for _ in range(SLOTS)],
        compiler_params=pltpu.CompilerParams(vmem_limit_bytes=40 * 1024 * 1024),
        name="attend",
    )(chosen, queries, table)


COLS = 512


def keep_body(peer_ref, x_ref, w_ref, out_ref):
    rows = out_ref.shape[0]
    x = x_ref[pl.ds(pl.multiple_of(peer_ref[0] * rows, rows), rows), :]
    for j in range(0, out_ref.shape[1], COLS):
        part = jnp.dot(x, w_ref[:, j : j + COLS], preferred_element_type=jnp.float32)
        out_ref[:, j : j + COLS] = part.astype(jnp.bfloat16)


def keep(peer, attended, w_out, rows):
    whole = pl.BlockSpec(memory_space=pltpu.VMEM)
    return pl.pallas_call(
        keep_body,
        in_specs=[pl.BlockSpec(memory_space=pltpu.SMEM), whole, whole],
        out_specs=whole,
        out_shape=jax.ShapeDtypeStruct((rows, w_out.shape[1]), jnp.bfloat16),
        compiler_params=pltpu.CompilerParams(vmem_limit_bytes=16 * 1024 * 1024),
        name="keep",
    )(peer, attended, w_out)


def combine_body(peer_ref, own_ref, x_ref, w_ref, out_ref):
    peers = x_ref.shape[0]
    others = [lax.rem(peer_ref[0] + away, peers) for away in range(1, peers)]
    parts = [x_ref[g] for g in others]
    for j in range(0, out_ref.shape[1], COLS):
        total = own_ref[:, j : j + COLS].astype(jnp.float32)
        for g, x in zip(others, parts):
            part = jnp.dot(x, w_ref[g, :, j : j + COLS], preferred_element_type=jnp.float32)
            total = total + part.astype(jnp.bfloat16).astype(jnp.float32)
        out_ref[:, j : j + COLS] = total.astype(jnp.bfloat16)


def combine(peer, own, parts, weights):
    whole = pl.BlockSpec(memory_space=pltpu.VMEM)
    return pl.pallas_call(
        combine_body,
        in_specs=[pl.BlockSpec(memory_space=pltpu.SMEM)] + [whole] * 3,
        out_specs=whole,
        out_shape=jax.ShapeDtypeStruct(own.shape, jnp.bfloat16),
        compiler_params=pltpu.CompilerParams(vmem_limit_bytes=16 * 1024 * 1024),
        name="combine",
    )(peer, own, parts, weights)


def rope_tables(row_count):
    blocks = row_count // BLOCK
    row = jnp.arange(blocks + BLOCK)
    start = lax.axis_index("kv") * row_count + row * BLOCK
    positions = jnp.where(row < blocks, start, row - blocks).astype(jnp.float32)
    lane = jnp.arange(LANES)
    freqs = ROPE_BASE ** (-(lane % HALF).astype(jnp.float32) / HALF)
    angles = positions[:, None] * freqs
    return jnp.cos(angles), jnp.sin(angles)


def exchange(tiles):
    return lax.all_to_all(tiles, "tp", split_axis=0, concat_axis=0, tiled=True)


def shards(tokens, w_query, w_key, w_value, w_out, selection):
    row_count = tokens.shape[0]
    peers = lax.axis_size("tp")
    peer = lax.axis_index("tp").reshape(1)
    cosine, sine = rope_tables(row_count)
    codes, w_sent = project_codes(tokens, w_key, w_value, cosine, sine, w_out, peers)
    weights = exchange(w_sent)
    queries = project_queries(tokens, w_query, cosine, sine)
    table = lax.all_gather(codes, "kv", axis=0, tiled=True)
    attended = attend(selection[0], queries, table)
    attended, weights = lax.optimization_barrier((attended, weights))
    arrived = exchange(attended.reshape(peers, row_count // peers, attended.shape[1]))
    own = keep(peer, attended, w_out, row_count // peers)
    return combine(peer, own, arrived, weights)


def solution(mesh):
    placed = (
        P(("grp", "kv"), None),
        P(None, "tp"),
        P(None, "tp"),
        P(None, "tp"),
        P("tp", None),
        P("tp", ("grp", "kv"), None),
    )
    return jax.shard_map(
        shards, mesh=mesh, in_specs=placed, out_specs=P(("grp", "kv", "tp"), None), check_vma=False
    )
```

```python
import jax
import jax.numpy as jnp
from jax import lax
from jax.experimental import pallas as pl
from jax.experimental.pallas import tpu as pltpu
from jax.sharding import PartitionSpec as P


HEAD_DIM = 64
BLOCK = 64
ROPE_BASE = 500000.0
LANES = 2 * HEAD_DIM
HALF = HEAD_DIM // 2


def encode(x):
    mag = jnp.abs(x)
    live = mag >= 2.0**-126
    safe = jnp.where(live, mag, 1.0)
    exponent = jnp.clip(jnp.floor(jnp.log2(safe)), -126.0, 126.0)
    half_exp = jnp.floor(exponent * 0.5)
    mantissa = safe * jnp.exp2(-half_exp) * jnp.exp2(half_exp - exponent)
    place = jnp.floor(mantissa * 128.0 - 127.5)
    carry = place >= 128.0
    place = jnp.where(carry, 0.0, place)
    exponent = jnp.where(carry, exponent + 1.0, exponent)
    code = (exponent + 1.0) * 256.0 + jnp.where(x < 0, 127.0 - place, 128.0 + place)
    return jnp.where(live, code, 128.0 - 126.0 * 256.0).astype(jnp.int32).astype(jnp.int16)


def decode(code):
    level = code.astype(jnp.int32).astype(jnp.float32) * (1.0 / 256.0)
    whole = jnp.floor(level)
    part = level - whole
    part = part - jnp.where(part < 0.5, 255.0 / 256.0, 0.0)
    return (part * jnp.exp2(whole)).astype(jnp.bfloat16)


def swap_halves(x, lane):
    return jnp.where(
        lane % HEAD_DIM < HALF,
        pltpu.roll(x, LANES - HALF, 1),
        pltpu.roll(x, HALF, 1),
    )


def turns(cos_ref, sin_ref, b):
    starts = cos_ref.shape[0] - BLOCK
    cos_at = cos_ref[b : b + 1, :]
    sin_at = sin_ref[b : b + 1, :]
    cos_in = cos_ref[starts:, :]
    sin_in = sin_ref[starts:, :]
    lane = lax.broadcasted_iota(jnp.int32, (BLOCK, LANES), 1)
    sign = jnp.where(lane % HEAD_DIM < HALF, -1.0, 1.0)
    return cos_at * cos_in - sin_at * sin_in, (sin_at * cos_in + cos_at * sin_in) * sign, lane


TILE = 4 * BLOCK
PART = 2 * BLOCK


def codes_body(
    tok_hbm, wk_hbm, wv_hbm, cos_hbm, sin_hbm, wo_hbm, code_hbm, sent_hbm,
    tok_ref, wkv_ref, cos_ref, sin_ref, code_ref, wo_ref, sems
):
    firsts = range(0, tok_ref.shape[0], PART)
    peers = sent_hbm.shape[0]
    at = iter(range(5 + 2 * len(firsts) + peers))
    small = [
        pltpu.make_async_copy(wk_hbm, wkv_ref.at[:HEAD_DIM], sems.at[next(at)]),
        pltpu.make_async_copy(wv_hbm, wkv_ref.at[HEAD_DIM:], sems.at[next(at)]),
        pltpu.make_async_copy(cos_hbm, cos_ref, sems.at[next(at)]),
        pltpu.make_async_copy(sin_hbm, sin_ref, sems.at[next(at)]),
    ]
    spans = [pl.ds(first, PART) for first in firsts]
    reads = [
        pltpu.make_async_copy(tok_hbm.at[span], tok_ref.at[span], sems.at[next(at)]) for span in spans
    ]
    writes = [
        pltpu.make_async_copy(code_ref.at[span], code_hbm.at[span], sems.at[next(at)]) for span in spans
    ]
    copies = [
        pltpu.make_async_copy(wo_ref, sent_hbm.at[peer], sems.at[next(at)]) for peer in range(peers)
    ]
    stage = pltpu.make_async_copy(wo_hbm, wo_ref, sems.at[next(at)])
    for move in small + reads[:1] + [stage] + reads[1:]:
        move.start()
    for move in small:
        move.wait()
    for first, read, write in zip(firsts, reads, writes):
        read.wait()
        if first == PART:
            stage.wait()
            for move in copies:
                move.start()
        kv_all = lax.dot_general(
            tok_ref[first : first + PART, :],
            wkv_ref[...],
            (((1,), (1,)), ((), ())),
            preferred_element_type=jnp.float32,
        )
        for at in range(0, PART, BLOCK):
            cosine, sine, lane = turns(cos_ref, sin_ref, (first + at) // BLOCK)
            kv = kv_all[at : at + BLOCK]
            kv = jnp.where(lane < HEAD_DIM, kv * cosine + swap_halves(kv, lane) * sine, kv)
            code_ref[first + at : first + at + BLOCK, :] = encode(
                kv.astype(jnp.bfloat16).astype(jnp.float32)
            )
        write.start()
    for move in writes + copies:
        move.wait()


def project_codes(tokens, w_key, w_value, cosine, sine, w_out, peers):
    rows, width = tokens.shape
    far = pl.BlockSpec(memory_space=pltpu.HBM)
    return pl.pallas_call(
        codes_body,
        in_specs=[far] * 6,
        out_specs=[far] * 2,
        out_shape=[
            jax.ShapeDtypeStruct((rows, LANES), jnp.int16),
            jax.ShapeDtypeStruct((peers, *w_out.shape), jnp.bfloat16),
        ],
        scratch_shapes=[
            pltpu.VMEM((rows, width), jnp.bfloat16),
            pltpu.VMEM((LANES, width), jnp.bfloat16),
            pltpu.VMEM(cosine.shape, jnp.float32),
            pltpu.VMEM(sine.shape, jnp.float32),
            pltpu.VMEM((rows, LANES), jnp.int16),
            pltpu.VMEM(w_out.shape, jnp.bfloat16),
            pltpu.SemaphoreType.DMA((5 + 2 * (rows // PART) + peers,)),
        ],
        compiler_params=pltpu.CompilerParams(vmem_limit_bytes=63 * 1024 * 1024),
        name="project_codes",
    )(tokens, w_key.T, w_value.T, cosine, sine, w_out)


def queries_body(tok_ref, wq_ref, cos_ref, sin_ref, q_ref):
    for first in range(0, tok_ref.shape[0], TILE):
        q_all = jnp.dot(
            tok_ref[first : first + TILE, :], wq_ref[...], preferred_element_type=jnp.float32
        )
        for at in range(0, TILE, BLOCK):
            b = (first + at) // BLOCK
            cosine, sine, lane = turns(cos_ref, sin_ref, b)
            for pair in range(q_all.shape[1] // LANES):
                q = q_all[at : at + BLOCK, pair * LANES : (pair + 1) * LANES]
                q = q * cosine + swap_halves(q, lane) * sine
                q = q.astype(jnp.bfloat16).astype(jnp.float32) * HEAD_DIM**-0.5
                even = 2 * pair * BLOCK
                odd = even + BLOCK
                q_ref[b, even:odd, :] = jnp.where(lane < HEAD_DIM, q, 0.0).astype(jnp.bfloat16)
                q_ref[b, odd : odd + BLOCK, :] = jnp.where(
                    lane < HEAD_DIM, pltpu.roll(q, HEAD_DIM, 1), 0.0
                ).astype(jnp.bfloat16)


def project_queries(tokens, w_query, cosine, sine):
    rows = tokens.shape[0]
    heads = w_query.shape[1] // HEAD_DIM
    whole = pl.BlockSpec(memory_space=pltpu.VMEM)
    return pl.pallas_call(
        queries_body,
        in_specs=[whole] * 4,
        out_specs=whole,
        out_shape=jax.ShapeDtypeStruct((rows // BLOCK, heads * BLOCK, LANES), jnp.bfloat16),
        compiler_params=pltpu.CompilerParams(vmem_limit_bytes=32 * 1024 * 1024),
        name="project_queries",
    )(tokens, w_query, cosine, sine)


SLOTS = 4


def attend_body(sel_ref, q_ref, table_ref, out_ref, *scratch):
    kv_refs, s_refs, p_refs = scratch[:SLOTS], scratch[SLOTS : 2 * SLOTS], scratch[2 * SLOTS :]
    blocks, topk = sel_ref.shape
    rows = q_ref.shape[1]
    keys = topk * BLOCK
    chunk = 16
    row = lax.broadcasted_iota(jnp.int32, (chunk, LANES), 0)
    col = lax.broadcasted_iota(jnp.int32, (chunk, LANES), 1)
    key_at = lax.broadcasted_iota(jnp.int32, (1, keys), 1)
    half_lane = lax.broadcasted_iota(jnp.int32, (BLOCK, LANES), 1) < HEAD_DIM

    def load(k, b):
        used = jnp.int32(0)
        for t in range(topk):
            block = sel_ref[b, t]
            used += (block >= 0).astype(jnp.int32)
            at = pl.multiple_of(jnp.maximum(block, 0) * BLOCK, BLOCK)
            kv_refs[k][t * BLOCK : (t + 1) * BLOCK, :] = decode(table_ref[pl.ds(at, BLOCK), :])
        return jnp.where(key_at < used * BLOCK, 0.0, -jnp.inf)

    def score(k, b):
        s_refs[k][...] = lax.dot_general(
            q_ref[b], kv_refs[k][...], (((1,), (1,)), ((), ())), preferred_element_type=jnp.float32
        )

    def soften(k, bias):
        sums = []
        for r in range(0, rows, chunk):
            s = s_refs[k][r : r + chunk, :] + bias
            first = jnp.where((col < BLOCK) & (col > row + r % BLOCK), -jnp.inf, s[:, :LANES])
            s = jnp.concatenate([first, s[:, LANES:]], axis=1)
            e = jnp.exp(s - jnp.max(s, axis=1, keepdims=True))
            sums.append(jnp.sum(e, axis=1, keepdims=True))
            p_refs[k][r : r + chunk, :] = e.astype(jnp.bfloat16)
        return jnp.concatenate(sums, axis=0)

    def finish(k, b, sums):
        o = jnp.dot(p_refs[k][...], kv_refs[k][...], preferred_element_type=jnp.float32) / sums
        at = pl.multiple_of(b * BLOCK, BLOCK)
        for pair in range(rows // BLOCK // 2):
            even = o[2 * pair * BLOCK : (2 * pair + 1) * BLOCK]
            odd = o[(2 * pair + 1) * BLOCK : (2 * pair + 2) * BLOCK]
            both = jnp.where(half_lane, pltpu.roll(even, HEAD_DIM, 1), odd)
            out_ref[pl.ds(at, BLOCK), pair * LANES : (pair + 1) * LANES] = both.astype(jnp.bfloat16)

    def step(i, _):
        first = i * SLOTS
        biases = [load(0, first)]
        score(0, first)
        for k in range(SLOTS):
            if k + 1 < SLOTS:
                biases.append(load(k + 1, first + k + 1))
            sums = soften(k, biases[k])
            if k + 1 < SLOTS:
                score(k + 1, first + k + 1)
            finish(k, first + k, sums)
        return 0

    lax.fori_loop(0, blocks // SLOTS, step, 0)


def attend(chosen, queries, table):
    blocks, topk = chosen.shape
    rows = queries.shape[1]
    cols = rows // BLOCK * HEAD_DIM
    keys = topk * BLOCK
    whole = pl.BlockSpec(memory_space=pltpu.VMEM)
    return pl.pallas_call(
        attend_body,
        in_specs=[pl.BlockSpec(memory_space=pltpu.SMEM), whole, whole],
        out_specs=whole,
        out_shape=jax.ShapeDtypeStruct((blocks * BLOCK, cols), jnp.bfloat16),
        scratch_shapes=[pltpu.VMEM((keys, LANES), jnp.bfloat16) for _ in range(SLOTS)]
        + [pltpu.VMEM((rows, keys), jnp.float32) for _ in range(SLOTS)]
        + [pltpu.VMEM((rows, keys), jnp.bfloat16) for _ in range(SLOTS)],
        compiler_params=pltpu.CompilerParams(vmem_limit_bytes=40 * 1024 * 1024),
        name="attend",
    )(chosen, queries, table)


COLS = 512


def keep_body(peer_ref, x_ref, w_ref, out_ref):
    rows = out_ref.shape[0]
    x = x_ref[pl.ds(pl.multiple_of(peer_ref[0] * rows, rows), rows), :]
    for j in range(0, out_ref.shape[1], COLS):
        part = jnp.dot(x, w_ref[:, j : j + COLS], preferred_element_type=jnp.float32)
        out_ref[:, j : j + COLS] = part.astype(jnp.bfloat16)


def keep(peer, attended, w_out, rows):
    whole = pl.BlockSpec(memory_space=pltpu.VMEM)
    return pl.pallas_call(
        keep_body,
        in_specs=[pl.BlockSpec(memory_space=pltpu.SMEM), whole, whole],
        out_specs=whole,
        out_shape=jax.ShapeDtypeStruct((rows, w_out.shape[1]), jnp.bfloat16),
        compiler_params=pltpu.CompilerParams(vmem_limit_bytes=16 * 1024 * 1024),
        name="keep",
    )(peer, attended, w_out)


def combine_body(peer_ref, own_ref, x_ref, all_hbm, out_ref, w_ref, sum_ref, sems):
    peers = x_ref.shape[0]
    others = [lax.rem(peer_ref[0] + away, peers) for away in range(1, peers)]
    moves = [
        pltpu.make_async_copy(all_hbm.at[g], w_ref.at[n], sems.at[n]) for n, g in enumerate(others)
    ]
    for move in moves:
        move.start()
    for n, (g, move) in enumerate(zip(others, moves)):
        x = x_ref[g]
        move.wait()
        for j in range(0, out_ref.shape[1], COLS):
            part = jnp.dot(x, w_ref[n, :, j : j + COLS], preferred_element_type=jnp.float32)
            before = own_ref[:, j : j + COLS].astype(jnp.float32) if n == 0 else sum_ref[:, j : j + COLS]
            total = before + part.astype(jnp.bfloat16).astype(jnp.float32)
            if n + 1 < len(others):
                sum_ref[:, j : j + COLS] = total
            else:
                out_ref[:, j : j + COLS] = total.astype(jnp.bfloat16)


def combine(peer, own, parts, weights):
    whole = pl.BlockSpec(memory_space=pltpu.VMEM)
    others = weights.shape[0] - 1
    return pl.pallas_call(
        combine_body,
        in_specs=[
            pl.BlockSpec(memory_space=pltpu.SMEM),
            whole,
            whole,
            pl.BlockSpec(memory_space=pltpu.HBM),
        ],
        out_specs=whole,
        out_shape=jax.ShapeDtypeStruct(own.shape, jnp.bfloat16),
        scratch_shapes=[
            pltpu.VMEM((others, *weights.shape[1:]), jnp.bfloat16),
            pltpu.VMEM(own.shape, jnp.float32),
            pltpu.SemaphoreType.DMA((others,)),
        ],
        compiler_params=pltpu.CompilerParams(vmem_limit_bytes=16 * 1024 * 1024),
        name="combine",
    )(peer, own, parts, weights)


def rope_tables(row_count):
    blocks = row_count // BLOCK
    row = jnp.arange(blocks + BLOCK)
    start = lax.axis_index("kv") * row_count + row * BLOCK
    positions = jnp.where(row < blocks, start, row - blocks).astype(jnp.float32)
    lane = jnp.arange(LANES)
    freqs = ROPE_BASE ** (-(lane % HALF).astype(jnp.float32) / HALF)
    angles = positions[:, None] * freqs
    return jnp.cos(angles), jnp.sin(angles)


def exchange(tiles):
    return lax.all_to_all(tiles, "tp", split_axis=0, concat_axis=0, tiled=True)


def shards(tokens, w_query, w_key, w_value, w_out, selection):
    row_count = tokens.shape[0]
    peers = lax.axis_size("tp")
    peer = lax.axis_index("tp").reshape(1)
    cosine, sine = rope_tables(row_count)
    codes, w_sent = project_codes(tokens, w_key, w_value, cosine, sine, w_out, peers)
    weights = exchange(w_sent)
    queries = project_queries(tokens, w_query, cosine, sine)
    table = lax.all_gather(codes, "kv", axis=0, tiled=True)
    attended = attend(selection[0], queries, table)
    attended, weights = lax.optimization_barrier((attended, weights))
    arrived = exchange(attended.reshape(peers, row_count // peers, attended.shape[1]))
    own = keep(peer, attended, w_out, row_count // peers)
    return combine(peer, own, arrived, weights)


def solution(mesh):
    placed = (
        P(("grp", "kv"), None),
        P(None, "tp"),
        P(None, "tp"),
        P(None, "tp"),
        P("tp", None),
        P("tp", ("grp", "kv"), None),
    )
    return jax.shard_map(
        shards, mesh=mesh, in_specs=placed, out_specs=P(("grp", "kv", "tp"), None), check_vma=False
    )
```

```python
import functools

import jax
import jax.numpy as jnp
from jax import lax
from jax.experimental import pallas as pl
from jax.experimental.pallas import tpu as pltpu
from jax.sharding import PartitionSpec as P


HEAD_DIM = 64
BLOCK = 64
ROPE_BASE = 500000.0
LANES = 2 * HEAD_DIM
HALF = HEAD_DIM // 2


def encode(x):
    mag = jnp.abs(x)
    live = mag >= 2.0**-126
    safe = jnp.where(live, mag, 1.0)
    exponent = jnp.clip(jnp.floor(jnp.log2(safe)), -126.0, 126.0)
    half_exp = jnp.floor(exponent * 0.5)
    mantissa = safe * jnp.exp2(-half_exp) * jnp.exp2(half_exp - exponent)
    place = jnp.floor(mantissa * 128.0 - 127.5)
    carry = place >= 128.0
    place = jnp.where(carry, 0.0, place)
    exponent = jnp.where(carry, exponent + 1.0, exponent)
    code = (exponent + 1.0) * 256.0 + jnp.where(x < 0, 127.0 - place, 128.0 + place)
    return jnp.where(live, code, 128.0 - 126.0 * 256.0).astype(jnp.int32).astype(jnp.int16)


def decode(code):
    level = code.astype(jnp.int32).astype(jnp.float32) * (1.0 / 256.0)
    whole = jnp.floor(level)
    part = level - whole
    part = part - jnp.where(part < 0.5, 255.0 / 256.0, 0.0)
    return (part * jnp.exp2(whole)).astype(jnp.bfloat16)


def swap_halves(x, lane):
    return jnp.where(
        lane % HEAD_DIM < HALF,
        pltpu.roll(x, LANES - HALF, 1),
        pltpu.roll(x, HALF, 1),
    )


def turns(cos_ref, sin_ref, b):
    starts = cos_ref.shape[0] - BLOCK
    cos_at = cos_ref[b : b + 1, :]
    sin_at = sin_ref[b : b + 1, :]
    cos_in = cos_ref[starts:, :]
    sin_in = sin_ref[starts:, :]
    lane = lax.broadcasted_iota(jnp.int32, (BLOCK, LANES), 1)
    sign = jnp.where(lane % HEAD_DIM < HALF, -1.0, 1.0)
    return cos_at * cos_in - sin_at * sin_in, (sin_at * cos_in + cos_at * sin_in) * sign, lane


TILE = 4 * BLOCK
PART = 2 * BLOCK


def codes_body(
    tok_hbm, wk_hbm, wv_hbm, cos_hbm, sin_hbm, wo_hbm, code_hbm, sent_hbm,
    tok_ref, wkv_ref, cos_ref, sin_ref, code_ref, wo_ref, sems
):
    firsts = range(0, tok_ref.shape[0], PART)
    peers = sent_hbm.shape[0]
    at = iter(range(5 + 2 * len(firsts) + peers))
    small = [
        pltpu.make_async_copy(wk_hbm, wkv_ref.at[:HEAD_DIM], sems.at[next(at)]),
        pltpu.make_async_copy(wv_hbm, wkv_ref.at[HEAD_DIM:], sems.at[next(at)]),
        pltpu.make_async_copy(cos_hbm, cos_ref, sems.at[next(at)]),
        pltpu.make_async_copy(sin_hbm, sin_ref, sems.at[next(at)]),
    ]
    spans = [pl.ds(first, PART) for first in firsts]
    reads = [
        pltpu.make_async_copy(tok_hbm.at[span], tok_ref.at[span], sems.at[next(at)]) for span in spans
    ]
    writes = [
        pltpu.make_async_copy(code_ref.at[span], code_hbm.at[span], sems.at[next(at)]) for span in spans
    ]
    copies = [
        pltpu.make_async_copy(wo_ref, sent_hbm.at[peer], sems.at[next(at)]) for peer in range(peers)
    ]
    stage = pltpu.make_async_copy(wo_hbm, wo_ref, sems.at[next(at)])
    for move in small + reads[:1] + [stage] + reads[1:]:
        move.start()
    for move in small:
        move.wait()
    for first, read, write in zip(firsts, reads, writes):
        read.wait()
        if first == PART:
            stage.wait()
            for move in copies:
                move.start()
        kv_all = lax.dot_general(
            tok_ref[first : first + PART, :],
            wkv_ref[...],
            (((1,), (1,)), ((), ())),
            preferred_element_type=jnp.float32,
        )
        for at in range(0, PART, BLOCK):
            cosine, sine, lane = turns(cos_ref, sin_ref, (first + at) // BLOCK)
            kv = kv_all[at : at + BLOCK]
            kv = jnp.where(lane < HEAD_DIM, kv * cosine + swap_halves(kv, lane) * sine, kv)
            code_ref[first + at : first + at + BLOCK, :] = encode(
                kv.astype(jnp.bfloat16).astype(jnp.float32)
            )
        write.start()
    for move in writes + copies:
        move.wait()


def project_codes(tokens, w_key, w_value, cosine, sine, w_out, peers):
    rows, width = tokens.shape
    far = pl.BlockSpec(memory_space=pltpu.HBM)
    return pl.pallas_call(
        codes_body,
        in_specs=[far] * 6,
        out_specs=[far] * 2,
        out_shape=[
            jax.ShapeDtypeStruct((rows, LANES), jnp.int16),
            jax.ShapeDtypeStruct((peers, *w_out.shape), jnp.bfloat16),
        ],
        scratch_shapes=[
            pltpu.VMEM((rows, width), jnp.bfloat16),
            pltpu.VMEM((LANES, width), jnp.bfloat16),
            pltpu.VMEM(cosine.shape, jnp.float32),
            pltpu.VMEM(sine.shape, jnp.float32),
            pltpu.VMEM((rows, LANES), jnp.int16),
            pltpu.VMEM(w_out.shape, jnp.bfloat16),
            pltpu.SemaphoreType.DMA((5 + 2 * (rows // PART) + peers,)),
        ],
        compiler_params=pltpu.CompilerParams(vmem_limit_bytes=63 * 1024 * 1024),
        name="project_codes",
    )(tokens, w_key.T, w_value.T, cosine, sine, w_out)


def queries_body(tok_ref, wq_ref, cos_ref, sin_ref, q_ref):
    for first in range(0, tok_ref.shape[0], TILE):
        q_all = jnp.dot(
            tok_ref[first : first + TILE, :], wq_ref[...], preferred_element_type=jnp.float32
        )
        for at in range(0, TILE, BLOCK):
            b = (first + at) // BLOCK
            cosine, sine, lane = turns(cos_ref, sin_ref, b)
            for pair in range(q_all.shape[1] // LANES):
                q = q_all[at : at + BLOCK, pair * LANES : (pair + 1) * LANES]
                q = q * cosine + swap_halves(q, lane) * sine
                q = q.astype(jnp.bfloat16).astype(jnp.float32) * HEAD_DIM**-0.5
                even = 2 * pair * BLOCK
                odd = even + BLOCK
                q_ref[b, even:odd, :] = jnp.where(lane < HEAD_DIM, q, 0.0).astype(jnp.bfloat16)
                q_ref[b, odd : odd + BLOCK, :] = jnp.where(
                    lane < HEAD_DIM, pltpu.roll(q, HEAD_DIM, 1), 0.0
                ).astype(jnp.bfloat16)


def project_queries(tokens, w_query, cosine, sine):
    rows = tokens.shape[0]
    heads = w_query.shape[1] // HEAD_DIM
    whole = pl.BlockSpec(memory_space=pltpu.VMEM)
    return pl.pallas_call(
        queries_body,
        in_specs=[whole] * 4,
        out_specs=whole,
        out_shape=jax.ShapeDtypeStruct((rows // BLOCK, heads * BLOCK, LANES), jnp.bfloat16),
        compiler_params=pltpu.CompilerParams(vmem_limit_bytes=32 * 1024 * 1024),
        name="project_queries",
    )(tokens, w_query, cosine, sine)


SLOTS = 4


def attend_body(sel_ref, q_ref, table_ref, out_ref, *scratch):
    kv_refs, s_refs, p_refs = scratch[:SLOTS], scratch[SLOTS : 2 * SLOTS], scratch[2 * SLOTS :]
    blocks, topk = sel_ref.shape
    rows = q_ref.shape[1]
    keys = topk * BLOCK
    chunk = 16
    row = lax.broadcasted_iota(jnp.int32, (chunk, LANES), 0)
    col = lax.broadcasted_iota(jnp.int32, (chunk, LANES), 1)
    key_at = lax.broadcasted_iota(jnp.int32, (1, keys), 1)
    half_lane = lax.broadcasted_iota(jnp.int32, (BLOCK, LANES), 1) < HEAD_DIM

    def load(k, b):
        used = jnp.int32(0)
        for t in range(topk):
            block = sel_ref[b, t]
            used += (block >= 0).astype(jnp.int32)
            at = pl.multiple_of(jnp.maximum(block, 0) * BLOCK, BLOCK)
            kv_refs[k][t * BLOCK : (t + 1) * BLOCK, :] = decode(table_ref[pl.ds(at, BLOCK), :])
        return jnp.where(key_at < used * BLOCK, 0.0, -jnp.inf)

    def score(k, b):
        s_refs[k][...] = lax.dot_general(
            q_ref[b], kv_refs[k][...], (((1,), (1,)), ((), ())), preferred_element_type=jnp.float32
        )

    def soften(k, bias):
        sums = []
        for r in range(0, rows, chunk):
            s = s_refs[k][r : r + chunk, :]
            s = s if bias is None else s + bias
            first = jnp.where((col < BLOCK) & (col > row + r % BLOCK), -jnp.inf, s[:, :LANES])
            s = jnp.concatenate([first, s[:, LANES:]], axis=1)
            e = jnp.exp(s - jnp.max(s, axis=1, keepdims=True))
            sums.append(jnp.sum(e, axis=1, keepdims=True))
            p_refs[k][r : r + chunk, :] = e.astype(jnp.bfloat16)
        return jnp.concatenate(sums, axis=0)

    def finish(k, b, sums):
        o = jnp.dot(p_refs[k][...], kv_refs[k][...], preferred_element_type=jnp.float32) / sums
        at = pl.multiple_of(b * BLOCK, BLOCK)
        for pair in range(rows // BLOCK // 2):
            even = o[2 * pair * BLOCK : (2 * pair + 1) * BLOCK]
            odd = o[(2 * pair + 1) * BLOCK : (2 * pair + 2) * BLOCK]
            both = jnp.where(half_lane, pltpu.roll(even, HEAD_DIM, 1), odd)
            out_ref[pl.ds(at, BLOCK), pair * LANES : (pair + 1) * LANES] = both.astype(jnp.bfloat16)

    def work(first, full):
        biases = [load(0, first)]
        score(0, first)
        for k in range(SLOTS):
            if k + 1 < SLOTS:
                biases.append(load(k + 1, first + k + 1))
            sums = soften(k, None if full else biases[k])
            if k + 1 < SLOTS:
                score(k + 1, first + k + 1)
            finish(k, first + k, sums)

    def step(i, _):
        first = i * SLOTS
        least = sel_ref[first, topk - 1]
        for k in range(1, SLOTS):
            least = jnp.minimum(least, sel_ref[first + k, topk - 1])
        pl.when(least >= 0)(functools.partial(work, first, True))
        pl.when(least < 0)(functools.partial(work, first, False))
        return 0

    lax.fori_loop(0, blocks // SLOTS, step, 0)


def attend(chosen, queries, table):
    blocks, topk = chosen.shape
    rows = queries.shape[1]
    cols = rows // BLOCK * HEAD_DIM
    keys = topk * BLOCK
    whole = pl.BlockSpec(memory_space=pltpu.VMEM)
    return pl.pallas_call(
        attend_body,
        in_specs=[pl.BlockSpec(memory_space=pltpu.SMEM), whole, whole],
        out_specs=whole,
        out_shape=jax.ShapeDtypeStruct((blocks * BLOCK, cols), jnp.bfloat16),
        scratch_shapes=[pltpu.VMEM((keys, LANES), jnp.bfloat16) for _ in range(SLOTS)]
        + [pltpu.VMEM((rows, keys), jnp.float32) for _ in range(SLOTS)]
        + [pltpu.VMEM((rows, keys), jnp.bfloat16) for _ in range(SLOTS)],
        compiler_params=pltpu.CompilerParams(vmem_limit_bytes=40 * 1024 * 1024),
        name="attend",
    )(chosen, queries, table)


COLS = 512


def keep_body(peer_ref, x_ref, w_ref, out_ref):
    rows = out_ref.shape[0]
    x = x_ref[pl.ds(pl.multiple_of(peer_ref[0] * rows, rows), rows), :]
    for j in range(0, out_ref.shape[1], COLS):
        part = jnp.dot(x, w_ref[:, j : j + COLS], preferred_element_type=jnp.float32)
        out_ref[:, j : j + COLS] = part.astype(jnp.bfloat16)


def keep(peer, attended, w_out, rows):
    whole = pl.BlockSpec(memory_space=pltpu.VMEM)
    return pl.pallas_call(
        keep_body,
        in_specs=[pl.BlockSpec(memory_space=pltpu.SMEM), whole, whole],
        out_specs=whole,
        out_shape=jax.ShapeDtypeStruct((rows, w_out.shape[1]), jnp.bfloat16),
        compiler_params=pltpu.CompilerParams(vmem_limit_bytes=16 * 1024 * 1024),
        name="keep",
    )(peer, attended, w_out)


def combine_body(peer_ref, own_ref, x_ref, all_hbm, out_ref, w_ref, sum_ref, sems):
    peers = x_ref.shape[0]
    others = [lax.rem(peer_ref[0] + away, peers) for away in range(1, peers)]
    moves = [
        pltpu.make_async_copy(all_hbm.at[g], w_ref.at[n], sems.at[n]) for n, g in enumerate(others)
    ]
    for move in moves:
        move.start()
    for n, (g, move) in enumerate(zip(others, moves)):
        x = x_ref[g]
        move.wait()
        for j in range(0, out_ref.shape[1], COLS):
            part = jnp.dot(x, w_ref[n, :, j : j + COLS], preferred_element_type=jnp.float32)
            before = own_ref[:, j : j + COLS].astype(jnp.float32) if n == 0 else sum_ref[:, j : j + COLS]
            total = before + part.astype(jnp.bfloat16).astype(jnp.float32)
            if n + 1 < len(others):
                sum_ref[:, j : j + COLS] = total
            else:
                out_ref[:, j : j + COLS] = total.astype(jnp.bfloat16)


def combine(peer, own, parts, weights):
    whole = pl.BlockSpec(memory_space=pltpu.VMEM)
    others = weights.shape[0] - 1
    return pl.pallas_call(
        combine_body,
        in_specs=[
            pl.BlockSpec(memory_space=pltpu.SMEM),
            whole,
            whole,
            pl.BlockSpec(memory_space=pltpu.HBM),
        ],
        out_specs=whole,
        out_shape=jax.ShapeDtypeStruct(own.shape, jnp.bfloat16),
        scratch_shapes=[
            pltpu.VMEM((others, *weights.shape[1:]), jnp.bfloat16),
            pltpu.VMEM(own.shape, jnp.float32),
            pltpu.SemaphoreType.DMA((others,)),
        ],
        compiler_params=pltpu.CompilerParams(vmem_limit_bytes=16 * 1024 * 1024),
        name="combine",
    )(peer, own, parts, weights)


def rope_tables(row_count):
    blocks = row_count // BLOCK
    row = jnp.arange(blocks + BLOCK)
    start = lax.axis_index("kv") * row_count + row * BLOCK
    positions = jnp.where(row < blocks, start, row - blocks).astype(jnp.float32)
    lane = jnp.arange(LANES)
    freqs = ROPE_BASE ** (-(lane % HALF).astype(jnp.float32) / HALF)
    angles = positions[:, None] * freqs
    return jnp.cos(angles), jnp.sin(angles)


def exchange(tiles):
    return lax.all_to_all(tiles, "tp", split_axis=0, concat_axis=0, tiled=True)


def shards(tokens, w_query, w_key, w_value, w_out, selection):
    row_count = tokens.shape[0]
    peers = lax.axis_size("tp")
    peer = lax.axis_index("tp").reshape(1)
    cosine, sine = rope_tables(row_count)
    codes, w_sent = project_codes(tokens, w_key, w_value, cosine, sine, w_out, peers)
    weights = exchange(w_sent)
    queries = project_queries(tokens, w_query, cosine, sine)
    table = lax.all_gather(codes, "kv", axis=0, tiled=True)
    attended = attend(selection[0], queries, table)
    attended, weights = lax.optimization_barrier((attended, weights))
    arrived = exchange(attended.reshape(peers, row_count // peers, attended.shape[1]))
    own = keep(peer, attended, w_out, row_count // peers)
    return combine(peer, own, arrived, weights)


def solution(mesh):
    placed = (
        P(("grp", "kv"), None),
        P(None, "tp"),
        P(None, "tp"),
        P(None, "tp"),
        P("tp", None),
        P("tp", ("grp", "kv"), None),
    )
    return jax.shard_map(
        shards, mesh=mesh, in_specs=placed, out_specs=P(("grp", "kv", "tp"), None), check_vma=False
    )
```
